256 devices in a mesh: grp: 2 (over y), st: 32 (over z, core), tp: 4 (over x).
Axes of the slice: x: 4, y: 2, z: 16, core: 2. Of those that a mesh axis runs over, the one named last changes fastest.
The devices are a block of a 4x16x16 slice.
Arguments:
- tokens: bfloat16 [32768, 2048], P(('grp', 'st'), 'tp'), parts along dimension 0, may hold values from -180 to 180
- ret_query: bfloat16 [32768, 1024], P(('grp', 'st'), 'tp'), parts along dimension 0, may hold values from -6 to 6
- ret_key: bfloat16 [32768, 1024], P(('grp', 'st'), 'tp'), parts along dimension 0, may hold values from -6 to 6
- ret_value: bfloat16 [32768, 1024], P(('grp', 'st'), 'tp'), parts along dimension 0, may hold values from -6 to 6
- w_query: bfloat16 [2048, 2048], P(None, 'tp'), may hold values from -0.125 to 0.125
- w_key: bfloat16 [2048, 2048], P(None, 'tp'), may hold values from -0.125 to 0.125
- w_value: bfloat16 [2048, 2048], P(None, 'tp'), may hold values from -0.125 to 0.125
- w_gate: bfloat16 [2048, 4], replicated, may hold values from -0.125 to 0.125
- store: bfloat16 [192, 128, 2048], P('st'), may hold values from -6 to 6
- passage_ids: int32 [512, 4], P(('grp', 'st')), parts along dimension 0, may hold values from 0 to 191, as said below
Outputs:
- blended: bfloat16 [32768, 3072], P(('grp', 'st'), 'tp'), parts along dimension 0
The draws below stay inside these ranges and needn't reach their ends.
There are 2 independent parts, one for each index of `grp`. The reference program is written for one: setup_inputs(seed, part) draws one part's arguments, and reference() takes and returns one part's arrays. A program takes and returns all parts, laid end to end along the dimension named above; an argument that names none is the same for every part. Nothing has to cross between parts.
Inputs may be any that keep to these rules, and one draw needn't show every extreme that they name: `passage_ids`: passage p lies on index p // 6 of st. The 8 rows of one device name passages of any one index of st at most 2 times in all, and those of some index exactly 2 times.
All inputs are finite; a program needn't handle non-finite values.
Results may differ from the reference program's by a relative error of at most 0.0094.
Values may be sent and summed in bfloat16 or wider, within the bound.
No kernel may reach another device: no remote copies, remote signals or barrier semaphores. Data moves between devices by JAX's collectives and lax.ppermute only.
A program may use at most 128 MiB of HBM per device.

```python
import jax
import jax.numpy as jnp
from jax import lax

D = 2048
HEADS = 4
RET_DIM = 256
HEAD_DIM = 512
PROWS = 128
BLOCK = 64
NPB = 4
TOK_DEV = 512
PASS_DEV = 6
SEQ_LEN = 256
TOKENS = 16384
BLK_DEV = 8
NBLK = 256
PASSAGES = 192
CAP = 2
N_ST = 32


def draw_tokens(key, part):
    layout = (TOK_DEV * N_ST, D)
    values = 1.5 * jax.random.truncated_normal(jax.random.fold_in(key, 11), -6.0, 6.0, layout, jnp.float32)
    return values.astype(jnp.bfloat16)


def requests_for(subkey, device):
    entries = jnp.arange(N_ST * CAP, dtype=jnp.int32)
    owner_of = entries // CAP
    copy_of = entries % CAP
    full_owner = (device + jax.random.randint(jax.random.fold_in(subkey, 1), (), 0, N_ST // 2)) % N_ST
    before_owner = (device + N_ST - 1) % N_ST
    across_owner = (device + N_ST // 2) % N_ST
    forced = (owner_of == full_owner) | (copy_of == 0) & ((owner_of == before_owner) | (owner_of == across_owner))
    popular = jax.random.randint(jax.random.fold_in(subkey, 2), (N_ST,), 0, 131072)
    jitter = jax.random.randint(jax.random.fold_in(subkey, 3), (N_ST * CAP,), 0, 32768)
    priority = jnp.where(forced, 524288, jnp.take(popular, owner_of) + jitter) * 1024 + entries
    _, chosen = lax.top_k(priority, BLK_DEV * NPB)
    within = jax.random.randint(jax.random.fold_in(subkey, 4), (BLK_DEV * NPB,), 0, PASS_DEV)
    picked = jnp.take(owner_of, chosen) * PASS_DEV + within
    return jax.random.permutation(jax.random.fold_in(subkey, 5), picked)


def draw_passage_ids(key, part):
    subkeys = jax.random.split(jax.random.fold_in(key, 21), N_ST)
    picked = jax.vmap(requests_for)(subkeys, jnp.arange(N_ST, dtype=jnp.int32))
    return picked.reshape(N_ST * BLK_DEV, NPB).astype(jnp.int32)


def level_of(rng, dims, cuts, least, high):
    def one(position, parts):
        steps = jax.random.uniform(jax.random.fold_in(jax.random.fold_in(rng, 6), position), (parts,), jnp.float32, least / len(cuts), high / len(cuts))
        return jnp.repeat(jnp.exp(steps), dims[position] // parts).reshape((-1,) + (1,) * (len(dims) - position - 1))

    gain = one(*cuts[0])
    for cut in cuts[1:]:
        gain = gain * one(*cut)
    return gain


def gaussian(own_key, extent, width, limit, shards=(), kind=jnp.bfloat16):
    gain = level_of(own_key, extent, shards, -0.22, 0.18) if shards else 1.0
    values = jax.random.normal(own_key, extent, jnp.float32) * width * gain
    return jnp.minimum(jnp.maximum(values, -limit), limit).astype(kind)


def setup_inputs(seed: int = 0, part: int = 0) -> dict:
    seeds = jax.random.split(jax.random.key(seed), 11)
    part_keys = jax.random.split(jax.random.fold_in(seeds[10], part), 11)
    return {
        "tokens": draw_tokens(jax.random.fold_in(jax.random.fold_in(seeds[10], part), 71), part),
        "ret_query": gaussian(part_keys[1], (TOKENS, HEADS * RET_DIM), 1.0, 6.0, ((0, 32), (1, 4))),
        "ret_key": gaussian(part_keys[2], (TOKENS, HEADS * RET_DIM), 1.0, 6.0, ((0, 32), (1, 4))),
        "ret_value": gaussian(part_keys[3], (TOKENS, HEADS * RET_DIM), 1.0, 6.0, ((0, 32), (1, 4))),
        "w_query": gaussian(seeds[4], (D, HEADS * HEAD_DIM), D ** -0.5, 0.125, ((1, 4),)),
        "w_key": gaussian(seeds[5], (D, HEADS * HEAD_DIM), D ** -0.5, 0.125, ((1, 4),)),
        "w_value": gaussian(seeds[6], (D, HEADS * HEAD_DIM), D ** -0.5, 0.125, ((1, 4),)),
        "w_gate": gaussian(seeds[7], (D, HEADS), D ** -0.5, 0.125),
        "store": gaussian(seeds[8], (PASSAGES, PROWS, D), 1.0, 6.0, ((0, 32),)),
        "passage_ids": draw_passage_ids(jax.random.fold_in(jax.random.fold_in(seeds[10], part), 71), part),
    }


ROTARY_BASE = 10000.0
NORM_EPS = 1e-05

def rounded(values):
    return lax.optimization_barrier(values.astype(jnp.bfloat16)).astype(jnp.float32)

def rotate(values, positions):
    halfway = values.shape[-1] // 2
    inverse = ROTARY_BASE ** (-jnp.arange(halfway, dtype=jnp.float32) / halfway)
    angles = positions.astype(jnp.float32)[:, None, None] * inverse
    cosines, sines = (jnp.cos(angles), jnp.sin(angles))
    leading, trailing = (values[..., :halfway], values[..., halfway:])
    return jnp.concatenate([leading * cosines - trailing * sines, leading * sines + trailing * cosines], axis=-1)

def retain_all(query_rows, key_rows, value_rows):
    layout = (TOKENS // SEQ_LEN, SEQ_LEN, HEADS, RET_DIM)
    places = jnp.arange(SEQ_LEN, dtype=jnp.int32)
    rot_query = rounded(rotate(query_rows.reshape(layout).astype(jnp.float32), places))
    rot_key = rounded(rotate(key_rows.reshape(layout).astype(jnp.float32), places) * RET_DIM ** (-0.5))
    head_number = jnp.arange(HEADS, dtype=jnp.float32)
    log_gamma = jnp.log1p(-jnp.exp2(-5.0 - head_number))
    offsets = (places[:, None] - places[None, :]).astype(jnp.float32)
    decays = jnp.where(offsets[None] >= 0.0, jnp.exp(log_gamma[:, None, None] * jnp.maximum(offsets, 0.0)[None]), 0.0)
    scores = jnp.einsum('sigd,sjgd->sgij', rot_query, rot_key)
    weights = rounded(scores * decays[None])
    output = jnp.einsum('sgij,sjge->sige', weights, value_rows.reshape(layout).astype(jnp.float32))
    centred = output - lax.optimization_barrier(jnp.mean(output, -1, keepdims=True))
    normed = centred * lax.rsqrt(lax.optimization_barrier(jnp.mean(centred * centred, -1, keepdims=True)) + NORM_EPS)
    return normed.astype(jnp.bfloat16).reshape(TOKENS, HEADS, RET_DIM)

def reference(tokens, ret_query, ret_key, ret_value, w_query, w_key, w_value, w_gate, store, passage_ids):
    retained = retain_all(ret_query, ret_key, ret_value)
    queries = jnp.dot(tokens, w_query, preferred_element_type=jnp.float32).astype(jnp.bfloat16)
    gate_vals = jax.nn.sigmoid(jnp.dot(tokens, w_gate, preferred_element_type=jnp.float32))
    keys_all = jnp.dot(store, w_key, preferred_element_type=jnp.float32).astype(jnp.bfloat16)
    values_all = jnp.dot(store, w_value, preferred_element_type=jnp.float32).astype(jnp.bfloat16)

    def attend(inputs):
        query_block, id_row, gate_block = inputs
        key_sel = jnp.take(keys_all, id_row, axis=0).reshape(NPB, PROWS, HEADS, HEAD_DIM).astype(jnp.float32)
        value_sel = jnp.take(values_all, id_row, axis=0).reshape(NPB, PROWS, HEADS, HEAD_DIM).astype(jnp.float32)
        scores = jnp.einsum('thd,jrhd->jhtr', query_block.astype(jnp.float32), key_sel) * HEAD_DIM ** (-0.5)
        highest = lax.optimization_barrier(jnp.max(scores, -1))
        exponent = jnp.exp(scores - highest[..., None])
        totals = lax.optimization_barrier(jnp.sum(exponent, -1))
        weighted = rounded(jnp.einsum('jhtr,jrhd->jthd', rounded(exponent), value_sel))
        overall = lax.optimization_barrier(jnp.max(highest, 0))
        scales = jnp.exp(highest - overall[None])
        denominator = lax.optimization_barrier(jnp.sum(scales * totals, 0))
        numerator = lax.optimization_barrier(jnp.sum(jnp.transpose(scales, (0, 2, 1))[..., None] * weighted, 0))
        return (gate_block[..., None] * numerator / jnp.transpose(denominator)[..., None]).astype(jnp.bfloat16)
    retrieved = lax.map(attend, (queries.reshape(NBLK, BLOCK, HEADS, HEAD_DIM), passage_ids, gate_vals.reshape(NBLK, BLOCK, HEADS)))
    retrieved = retrieved.reshape(TOKENS, HEADS, HEAD_DIM)
    return jnp.concatenate([retained, retrieved], -1).reshape(TOKENS, HEADS * (RET_DIM + HEAD_DIM))
```

```python
import functools

import jax
import jax.numpy as jnp
from jax import lax
from jax.experimental import pallas as pl
from jax.experimental.pallas import tpu as pltpu
from jax.sharding import PartitionSpec as P

RET_DIM = 256
HEAD_DIM = 512
BLOCK = 64
NPB = 4
SEQ_LEN = 256
PAIR = 2 * BLOCK
STATS = 16
LOWEST = -(2.0**127)

ROTARY_BASE = 10000.0
NORM_EPS = 1e-05


def rotate(values, positions):
    halfway = values.shape[-1] // 2
    inverse = ROTARY_BASE ** (-jnp.arange(halfway, dtype=jnp.float32) / halfway)
    angles = positions.astype(jnp.float32)[:, None, None] * inverse
    cosines, sines = (jnp.cos(angles), jnp.sin(angles))
    leading, trailing = (values[..., :halfway], values[..., halfway:])
    return jnp.concatenate(
        [leading * cosines - trailing * sines, leading * sines + trailing * cosines], axis=-1
    )


def retain(query_rows, key_rows, value_rows, head_start):
    token_count = query_rows.shape[0]
    groups = query_rows.shape[1] // RET_DIM
    layout = (token_count // SEQ_LEN, SEQ_LEN, groups, RET_DIM)
    places = jnp.arange(SEQ_LEN, dtype=jnp.int32)
    rot_query = rotate(query_rows.reshape(layout).astype(jnp.float32), places).astype(jnp.bfloat16)
    rot_key = (
        rotate(key_rows.reshape(layout).astype(jnp.float32), places) * RET_DIM ** (-0.5)
    ).astype(jnp.bfloat16)
    head_number = (head_start + jnp.arange(groups, dtype=jnp.int32)).astype(jnp.float32)
    log_gamma = jnp.log1p(-jnp.exp2(-5.0 - head_number))
    offsets = (places[:, None] - places[None, :]).astype(jnp.float32)
    decays = jnp.where(
        offsets[None] >= 0.0,
        jnp.exp(log_gamma[:, None, None] * jnp.maximum(offsets, 0.0)[None]),
        0.0,
    )
    scores = jnp.einsum("sigd,sjgd->sgij", rot_query, rot_key, preferred_element_type=jnp.float32)
    weights = (scores * decays[None]).astype(jnp.bfloat16)
    output = jnp.einsum(
        "sgij,sjge->sige", weights, value_rows.reshape(layout), preferred_element_type=jnp.float32
    )
    centred = output - jnp.mean(output, -1, keepdims=True)
    normed = centred * lax.rsqrt(jnp.mean(centred * centred, -1, keepdims=True) + NORM_EPS)
    return normed.astype(jnp.bfloat16).reshape(token_count, groups * RET_DIM)


def split_three(row):
    high = row.astype(jnp.bfloat16).astype(jnp.float32)
    rest = row - high
    middle = rest.astype(jnp.bfloat16).astype(jnp.float32)
    return [high, middle, rest - middle]


def write_stats(out_ref, pairs, highest, totals):
    place = lax.broadcasted_iota(jnp.int32, (STATS, PAIR), 0)
    packed = jnp.zeros((STATS, PAIR), jnp.float32)
    row = 0
    for pair in range(pairs):
        for part in split_three(highest[pair]) + split_three(totals[pair]):
            packed = jnp.where(place == row, part, packed)
            row += 1
    out_ref[pairs * HEAD_DIM :, :] = packed.astype(jnp.bfloat16)


def read_stats(ref, pairs):
    packed = ref[pairs * HEAD_DIM :, :].astype(jnp.float32)
    rows = [packed[r : r + 1, :] for r in range(6 * pairs)]
    highest = [(rows[6 * p] + rows[6 * p + 1]) + rows[6 * p + 2] for p in range(pairs)]
    totals = [(rows[6 * p + 3] + rows[6 * p + 4]) + rows[6 * p + 5] for p in range(pairs)]
    return highest, totals


def contrib_kernel(offset, pairs, table_ref, query_ref, key_ref, value_ref, out_ref, acc, high, tot):
    acc[...] = jnp.zeros_like(acc)
    high[...] = jnp.full_like(high, LOWEST)
    tot[...] = jnp.zeros_like(tot)
    lane_block = lax.broadcasted_iota(jnp.int32, (1, PAIR), 1) // BLOCK

    def step(j, carry):
        passage = table_ref[offset + j]

        @pl.when(passage >= 0)
        def _():
            pair = j // (2 * NPB)
            mine = lane_block == (j // NPB) % 2
            query = query_ref[pl.ds(pl.multiple_of(pair * HEAD_DIM, HEAD_DIM), HEAD_DIM), :]
            rows = pl.multiple_of(passage * 128, 128)
            scores = jnp.dot(
                key_ref[pl.ds(rows, 128), :], query, preferred_element_type=jnp.float32
            ) * HEAD_DIM ** (-0.5)
            top = jnp.max(scores, 0, keepdims=True)
            exponent = jnp.exp(scores - top)
            total = jnp.sum(exponent, 0, keepdims=True)
            weighted = jnp.dot(
                value_ref[:, pl.ds(rows, 128)],
                jnp.where(mine, exponent, 0.0).astype(jnp.bfloat16),
                preferred_element_type=jnp.float32,
            )
            at = pl.ds(pl.multiple_of(pair * 8, 8), 1)
            old = high[at, :]
            new = jnp.where(mine, jnp.maximum(old, top), old)
            keep = jnp.exp(old - new)
            take = jnp.where(mine, jnp.exp(top - new), 0.0)
            where = pl.ds(pl.multiple_of(pair * HEAD_DIM, HEAD_DIM), HEAD_DIM)
            acc[where, :] = acc[where, :] * keep + weighted * take
            high[at, :] = new
            tot[at, :] = tot[at, :] * keep + total * take

        return carry

    lax.fori_loop(0, 2 * pairs * NPB, step, 0)
    out_ref[: pairs * HEAD_DIM, :] = acc[...].astype(jnp.bfloat16)
    write_stats(
        out_ref,
        pairs,
        [high[8 * p : 8 * p + 1, :] for p in range(pairs)],
        [tot[8 * p : 8 * p + 1, :] for p in range(pairs)],
    )


def contribution(table, query, keys, values, offset, pairs):
    return pl.pallas_call(
        functools.partial(contrib_kernel, offset, pairs),
        out_shape=jax.ShapeDtypeStruct((pairs * HEAD_DIM + STATS, PAIR), jnp.bfloat16),
        in_specs=[
            pl.BlockSpec(memory_space=pltpu.SMEM),
            pl.BlockSpec(memory_space=pltpu.VMEM),
            pl.BlockSpec(memory_space=pltpu.VMEM),
            pl.BlockSpec(memory_space=pltpu.VMEM),
        ],
        out_specs=pl.BlockSpec(memory_space=pltpu.VMEM),
        scratch_shapes=[
            pltpu.VMEM((pairs * HEAD_DIM, PAIR), jnp.float32),
            pltpu.VMEM((8 * pairs, PAIR), jnp.float32),
            pltpu.VMEM((8 * pairs, PAIR), jnp.float32),
        ],
        cost_estimate=pl.CostEstimate(
            flops=2 * 10**9, transcendentals=10**5, bytes_accessed=10**6
        ),
        name="contribution",
    )(table, query, keys, values)


def merge_kernel(pairs, first_ref, second_ref, out_ref):
    high_a, tot_a = read_stats(first_ref, pairs)
    high_b, tot_b = read_stats(second_ref, pairs)
    highest, totals = [], []
    for p in range(pairs):
        top = jnp.maximum(high_a[p], high_b[p])
        scale_a, scale_b = jnp.exp(high_a[p] - top), jnp.exp(high_b[p] - top)
        rows = slice(p * HEAD_DIM, (p + 1) * HEAD_DIM)
        out_ref[rows, :] = (
            first_ref[rows, :].astype(jnp.float32) * scale_a
            + second_ref[rows, :].astype(jnp.float32) * scale_b
        ).astype(jnp.bfloat16)
        highest.append(top)
        totals.append(tot_a[p] * scale_a + tot_b[p] * scale_b)
    write_stats(out_ref, pairs, highest, totals)


def merged(first, second, pairs):
    return pl.pallas_call(
        functools.partial(merge_kernel, pairs),
        out_shape=jax.ShapeDtypeStruct(first.shape, first.dtype),
        in_specs=[pl.BlockSpec(memory_space=pltpu.VMEM)] * 2,
        out_specs=pl.BlockSpec(memory_space=pltpu.VMEM),
        cost_estimate=pl.CostEstimate(
            flops=10**9, transcendentals=10**4, bytes_accessed=10**6
        ),
        name="merge",
    )(first, second)


def final_kernel(pairs, *refs):
    message_refs, gate_ref, retained_ref, out_ref = refs[:-3], refs[-3], refs[-2], refs[-1]
    out_ref[:, :RET_DIM] = retained_ref[...]
    for half in range(len(message_refs) // 3):
        trio = message_refs[3 * half : 3 * half + 3]
        stats = [read_stats(ref, pairs) for ref in trio]
        for p in range(pairs):
            top = functools.reduce(jnp.maximum, [s[0][p] for s in stats])
            scales = [jnp.exp(s[0][p] - top) for s in stats]
            total = sum(s[1][p] * scale for s, scale in zip(stats, scales))
            tokens = slice((half * pairs + p) * PAIR, (half * pairs + p + 1) * PAIR)
            factor = gate_ref[:, tokens] / total
            for c in range(0, HEAD_DIM, 128):
                rows = slice(p * HEAD_DIM + c, p * HEAD_DIM + c + 128)
                value = sum(ref[rows, :].astype(jnp.float32) * scale for ref, scale in zip(trio, scales))
                out_ref[tokens, RET_DIM + c : RET_DIM + c + 128] = jnp.transpose(
                    value * factor
                ).astype(jnp.bfloat16)


def finished(messages, gate, retained, pairs):
    tokens = retained.shape[0]
    return pl.pallas_call(
        functools.partial(final_kernel, pairs),
        out_shape=jax.ShapeDtypeStruct((tokens, RET_DIM + HEAD_DIM), jnp.bfloat16),
        in_specs=[pl.BlockSpec(memory_space=pltpu.VMEM)] * (len(messages) + 2),
        out_specs=pl.BlockSpec(memory_space=pltpu.VMEM),
        name="finish",
    )(*messages, gate, retained)


def body(
    tokens, ret_query, ret_key, ret_value, w_query, w_key, w_value, w_gate, store, passage_ids
):
    owners = lax.axis_size("st")
    chips = owners // 2
    far = chips // 2
    columns = lax.axis_size("tp")
    head = lax.axis_index("tp")
    mine = lax.axis_index("st")
    held = store.shape[0]
    features = tokens.shape[1]
    token_count = tokens.shape[0]
    half_tokens = token_count // 2
    pairs = half_tokens // PAIR

    def along(x, hops):
        return lax.ppermute(x, "st", [(i, (i + 2 * hops) % owners) for i in range(owners)])

    def across(x, hops):
        return lax.ppermute(x, "tp", [(i, (i + hops) % columns) for i in range(columns)])

    ids = passage_ids.reshape(-1)
    reach = 1
    while reach < chips:
        ids = jnp.concatenate([ids, along(ids, -reach)])
        reach *= 2
    own_place = ids - mine * held
    other_place = ids - (mine ^ 1) * held
    table = jnp.where(
        (own_place >= 0) & (own_place < held),
        own_place,
        jnp.where((other_place >= 0) & (other_place < held), other_place + held, -1),
    )
    per_half = passage_ids.size // 2

    weight_rows = [
        lax.dynamic_slice_in_dim(w_query, ((head + k) % columns) * features, features, 0)
        for k in range(columns)
    ]
    gate_rows = [
        lax.dynamic_slice(
            w_gate, (((head + k) % columns) * features, head), (features, 1)
        )
        for k in range(columns)
    ]

    def times(weights, piece):
        return lax.dot_general(
            weights, piece, (((0,), (1,)), ((), ())), preferred_element_type=jnp.float32
        )

    queries, gates = [], []
    for half in range(2):
        piece = tokens[half * half_tokens : (half + 1) * half_tokens]
        before, after = across(piece, 1), across(piece, -1)
        opposite = [
            across(before[:PAIR], 1),
            across(after[PAIR:], -1),
        ]
        near = (
            times(weight_rows[0], piece)
            + times(weight_rows[3], before)
            + times(weight_rows[1], after)
        )
        queries.append(
            jnp.concatenate(
                [
                    (near[:, p * PAIR : (p + 1) * PAIR] + times(weight_rows[2], opposite[p])).astype(
                        jnp.bfloat16
                    )
                    for p in range(pairs)
                ]
            )
        )
        gates.append(
            times(gate_rows[0], piece)
            + times(gate_rows[3], before)
            + times(gate_rows[1], after)
            + jnp.concatenate([times(gate_rows[2], part) for part in opposite], 1)
        )
    gate = jax.nn.sigmoid(jnp.concatenate(gates, 1))

    store_rows = store.reshape(-1, store.shape[2])
    key_own = jnp.dot(store_rows, w_key, preferred_element_type=jnp.float32).astype(jnp.bfloat16)
    value_own = times(w_value, store_rows).astype(jnp.bfloat16)
    partner = [(i, i ^ 1) for i in range(owners)]
    keys = jnp.concatenate([key_own, lax.ppermute(key_own, "st", partner)], 0)
    values = jnp.concatenate([value_own, lax.ppermute(value_own, "st", partner)], 1)

    def contribute(query, distance, half):
        offset = (distance % chips) * 2 * per_half + half * per_half
        return contribution(table, query, keys, values, offset, pairs)

    parts = [{0: contribute(queries[half], 0, half)} for half in range(2)]
    streams = [(half, way) for half in range(2) for way in (1, -1)]
    longest = {(0, 1): far, (0, -1): far - 1, (1, 1): far - 1, (1, -1): far}
    moving = {s: queries[s[0]] for s in streams}
    for hop in range(1, far + 1):
        for half, way in streams:
            if hop <= longest[half, way]:
                moving[half, way] = along(moving[half, way], way)
                distance = (-way * hop) % chips
                parts[half][distance] = contribute(moving[half, way], distance, half)

    back = {}
    for left in range(far, 0, -1):
        for half, way in streams:
            if left > longest[half, way]:
                continue
            own = parts[half][(way * left) % chips]
            back[half, way] = along(
                merged(back[half, way], own, pairs) if (half, way) in back else own, way
            )

    retained = retain(ret_query, ret_key, ret_value, head)
    messages = []
    for half in range(2):
        messages += [back[half, 1], back[half, -1], parts[half][0]]
    return finished(messages, gate, retained, pairs)


def solution(mesh):
    placed = (
        P(("grp", "st"), "tp"),
        P(("grp", "st"), "tp"),
        P(("grp", "st"), "tp"),
        P(("grp", "st"), "tp"),
        P(None, "tp"),
        P(None, "tp"),
        P(None, "tp"),
        P(),
        P("st", None, None),
        P(("grp", "st"), None),
    )
    return jax.shard_map(
        body, mesh=mesh, in_specs=placed, out_specs=P(("grp", "st"), "tp"), check_vma=False
    )
```

```python
import functools

import jax
import jax.numpy as jnp
from jax import lax
from jax.experimental import pallas as pl
from jax.experimental.pallas import tpu as pltpu
from jax.sharding import PartitionSpec as P

RET_DIM = 256
HEAD_DIM = 512
BLOCK = 64
NPB = 4
SEQ_LEN = 256
PAIR = 2 * BLOCK
STATS = 16
LOWEST = -(2.0**127)

ROTARY_BASE = 10000.0
NORM_EPS = 1e-05


MIB = 1024 * 1024


def limited(mib):
    return pltpu.CompilerParams(vmem_limit_bytes=mib * MIB)


def in_vmem(count):
    return [pl.BlockSpec(memory_space=pltpu.VMEM)] * count


def after(x, *others):
    return lax.optimization_barrier((x, *others))[0]


def contracted(left, right, dims):
    return lax.dot_general(left, right, ((dims[:1], dims[1:]), ((), ())), preferred_element_type=jnp.float32)


def retain_kernel(cos_ref, sin_ref, decay_ref, query_ref, key_ref, value_ref, out_ref):
    half = RET_DIM // 2
    cosines, sines = cos_ref[...], sin_ref[...]

    def rotated(ref):
        values = ref[...].astype(jnp.float32)
        leading, trailing = values[:, :half], values[:, half:]
        return jnp.concatenate(
            [leading * cosines - trailing * sines, leading * sines + trailing * cosines], axis=1
        )

    query = rotated(query_ref).astype(jnp.bfloat16)
    key = (rotated(key_ref) * RET_DIM ** (-0.5)).astype(jnp.bfloat16)
    weights = (contracted(query, key, (1, 1)) * decay_ref[...]).astype(jnp.bfloat16)
    output = jnp.dot(weights, value_ref[...], preferred_element_type=jnp.float32)
    centred = output - jnp.mean(output, -1, keepdims=True)
    out_ref[...] = (
        centred * lax.rsqrt(jnp.mean(centred * centred, -1, keepdims=True) + NORM_EPS)
    ).astype(jnp.bfloat16)


def retention_tables(head):
    places = jnp.arange(SEQ_LEN, dtype=jnp.int32)
    half = RET_DIM // 2
    inverse = ROTARY_BASE ** (-jnp.arange(half, dtype=jnp.float32) / half)
    angles = places.astype(jnp.float32)[:, None] * inverse
    log_gamma = jnp.log1p(-jnp.exp2(-5.0 - head.astype(jnp.float32)))
    offsets = (places[:, None] - places[None, :]).astype(jnp.float32)
    decay = jnp.where(offsets >= 0.0, jnp.exp(log_gamma * jnp.maximum(offsets, 0.0)), 0.0)
    return jnp.cos(angles), jnp.sin(angles), decay


def retain(tables, query_rows, key_rows, value_rows):
    rows = pl.BlockSpec((SEQ_LEN, RET_DIM), lambda i: (i, 0))
    half = pl.BlockSpec((SEQ_LEN, RET_DIM // 2), lambda i: (0, 0))
    return pl.pallas_call(
        retain_kernel,
        grid=(query_rows.shape[0] // SEQ_LEN,),
        out_shape=jax.ShapeDtypeStruct(query_rows.shape, jnp.bfloat16),
        in_specs=[half, half, pl.BlockSpec((SEQ_LEN, SEQ_LEN), lambda i: (0, 0)), rows, rows, rows],
        out_specs=rows,
        compiler_params=limited(8),
        cost_estimate=pl.CostEstimate(flops=4 * 10**9, transcendentals=0, bytes_accessed=10**6),
        name="retain",
    )(*tables, query_rows, key_rows, value_rows)


def project_kernel(columns, head_ref, *refs):
    piece_refs, weight_ref, gate_weight_ref, query_ref, gate_ref = (
        refs[:columns], refs[-4], refs[-3], refs[-2], refs[-1]
    )
    features = piece_refs[0].shape[1]
    head = head_ref[0]
    total, gates = None, None
    for ref, away in zip(piece_refs, (0, columns - 1, 1, 2)):
        at = pl.ds(pl.multiple_of(lax.rem(head + away, columns) * features, features), features)
        piece = ref[...]
        part = jnp.dot(piece, weight_ref[at, :], preferred_element_type=jnp.float32)
        gate_part = contracted(gate_weight_ref[:, at], piece, (1, 1))
        total = part if total is None else total + part
        gates = gate_part if gates is None else gates + gate_part
    query_ref[...] = total.astype(jnp.bfloat16)
    which = lax.broadcasted_iota(jnp.int32, gates.shape, 0) == head
    gate_ref[...] = jax.nn.sigmoid(jnp.sum(jnp.where(which, gates, 0.0), 0, keepdims=True))


def project(head, pieces, weights, gate_weights):
    rows = pieces[0].shape[0]
    return pl.pallas_call(
        functools.partial(project_kernel, len(pieces)),
        out_shape=(
            jax.ShapeDtypeStruct((rows, weights.shape[1]), jnp.bfloat16),
            jax.ShapeDtypeStruct((1, rows), jnp.float32),
        ),
        in_specs=[pl.BlockSpec(memory_space=pltpu.SMEM)] + in_vmem(len(pieces) + 2),
        out_specs=tuple(in_vmem(2)),
        compiler_params=limited(8),
        cost_estimate=pl.CostEstimate(flops=2 * 10**9, transcendentals=0, bytes_accessed=10**6),
        name="project",
    )(head.reshape(1), *pieces, weights, gate_weights)


def split_three(row):
    high = row.astype(jnp.bfloat16).astype(jnp.float32)
    rest = row - high
    middle = rest.astype(jnp.bfloat16).astype(jnp.float32)
    return [high, middle, rest - middle]


def write_stats(out_ref, pairs, highest, totals):
    place = lax.broadcasted_iota(jnp.int32, (STATS, PAIR), 0)
    packed = jnp.zeros((STATS, PAIR), jnp.float32)
    row = 0
    for pair in range(pairs):
        for part in split_three(highest[pair]) + split_three(totals[pair]):
            packed = jnp.where(place == row, part, packed)
            row += 1
    out_ref[pairs * HEAD_DIM :, :] = packed.astype(jnp.bfloat16)


def read_stats(ref, pairs):
    packed = ref[pairs * HEAD_DIM :, :].astype(jnp.float32)
    rows = [packed[r : r + 1, :] for r in range(6 * pairs)]
    highest = [(rows[6 * p] + rows[6 * p + 1]) + rows[6 * p + 2] for p in range(pairs)]
    totals = [(rows[6 * p + 3] + rows[6 * p + 4]) + rows[6 * p + 5] for p in range(pairs)]
    return highest, totals


def contrib_kernel(offset, pairs, table_ref, query_ref, key_ref, value_ref, out_ref, high, tot):
    high[...] = jnp.full_like(high, LOWEST)
    tot[...] = jnp.zeros_like(tot)
    lane_block = lax.broadcasted_iota(jnp.int32, (1, PAIR), 1) // BLOCK

    def clear(i, carry):
        at = pl.ds(pl.multiple_of(i * 128, 128), 128)
        out_ref[at, :] = jnp.zeros((128, PAIR), jnp.bfloat16)
        return carry

    lax.fori_loop(0, pairs * HEAD_DIM // 128, clear, 0)

    def step(j, carry):
        passage = table_ref[offset + j]

        @pl.when(passage >= 0)
        def _():
            pair = j // (2 * NPB)
            mine = lane_block == (j // NPB) % 2
            rows = pl.multiple_of(passage * 128, 128)
            scores = contracted(
                key_ref[pl.ds(rows, 128), :],
                query_ref[pl.ds(pl.multiple_of(pair * PAIR, PAIR), PAIR), :],
                (1, 1),
            ) * HEAD_DIM ** (-0.5)
            top = jnp.max(scores, 0, keepdims=True)
            exponent = jnp.exp(scores - top)
            total = jnp.sum(exponent, 0, keepdims=True)
            weighted = jnp.dot(
                value_ref[:, pl.ds(rows, 128)],
                jnp.where(mine, exponent, 0.0).astype(jnp.bfloat16),
                preferred_element_type=jnp.float32,
            )
            at = pl.ds(pl.multiple_of(pair * 8, 8), 1)
            old = high[at, :]
            new = jnp.where(mine, jnp.maximum(old, top), old)
            keep = jnp.exp(old - new)
            take = jnp.where(mine, jnp.exp(top - new), 0.0)
            where = pl.ds(pl.multiple_of(pair * HEAD_DIM, HEAD_DIM), HEAD_DIM)
            out_ref[where, :] = (
                out_ref[where, :].astype(jnp.float32) * keep + weighted * take
            ).astype(jnp.bfloat16)
            high[at, :] = new
            tot[at, :] = tot[at, :] * keep + total * take

        return carry

    lax.fori_loop(0, 2 * pairs * NPB, step, 0)
    write_stats(
        out_ref,
        pairs,
        [high[8 * p : 8 * p + 1, :] for p in range(pairs)],
        [tot[8 * p : 8 * p + 1, :] for p in range(pairs)],
    )


def contribution(table, query, keys, values, offset, pairs):
    return pl.pallas_call(
        functools.partial(contrib_kernel, offset, pairs),
        out_shape=jax.ShapeDtypeStruct((pairs * HEAD_DIM + STATS, PAIR), jnp.bfloat16),
        in_specs=[pl.BlockSpec(memory_space=pltpu.SMEM)] + in_vmem(3),
        out_specs=in_vmem(1)[0],
        scratch_shapes=[
            pltpu.VMEM((8 * pairs, PAIR), jnp.float32),
            pltpu.VMEM((8 * pairs, PAIR), jnp.float32),
        ],
        compiler_params=limited(6),
        cost_estimate=pl.CostEstimate(
            flops=2 * 10**9, transcendentals=10**5, bytes_accessed=10**6
        ),
        name="contribution",
    )(table, query, keys, values)


def merge_kernel(pairs, first_ref, second_ref, out_ref):
    high_a, tot_a = read_stats(first_ref, pairs)
    high_b, tot_b = read_stats(second_ref, pairs)
    highest, totals = [], []
    for p in range(pairs):
        top = jnp.maximum(high_a[p], high_b[p])
        scale_a, scale_b = jnp.exp(high_a[p] - top), jnp.exp(high_b[p] - top)

        def blend(i, carry, p=p, scale_a=scale_a, scale_b=scale_b):
            rows = pl.ds(pl.multiple_of(p * HEAD_DIM + i * 128, 128), 128)
            out_ref[rows, :] = (
                first_ref[rows, :].astype(jnp.float32) * scale_a
                + second_ref[rows, :].astype(jnp.float32) * scale_b
            ).astype(jnp.bfloat16)
            return carry

        lax.fori_loop(0, HEAD_DIM // 128, blend, 0)
        highest.append(top)
        totals.append(tot_a[p] * scale_a + tot_b[p] * scale_b)
    write_stats(out_ref, pairs, highest, totals)


def merged(first, second, pairs):
    return pl.pallas_call(
        functools.partial(merge_kernel, pairs),
        out_shape=jax.ShapeDtypeStruct(first.shape, first.dtype),
        in_specs=in_vmem(2),
        out_specs=in_vmem(1)[0],
        compiler_params=limited(2),
        cost_estimate=pl.CostEstimate(
            flops=10**9, transcendentals=10**4, bytes_accessed=10**6
        ),
        name="merge",
    )(first, second)


def final_kernel(pairs, *refs):
    message_refs, gate_ref, retained_ref, out_ref = refs[:-3], refs[-3], refs[-2], refs[-1]
    out_ref[:, :RET_DIM] = retained_ref[...]
    for half in range(len(message_refs) // 3):
        trio = message_refs[3 * half : 3 * half + 3]
        stats = [read_stats(ref, pairs) for ref in trio]
        for p in range(pairs):
            top = functools.reduce(jnp.maximum, [s[0][p] for s in stats])
            scales = [jnp.exp(s[0][p] - top) for s in stats]
            total = sum(s[1][p] * scale for s, scale in zip(stats, scales))
            tokens = slice((half * pairs + p) * PAIR, (half * pairs + p + 1) * PAIR)
            factor = gate_ref[:, tokens] / total
            for c in range(0, HEAD_DIM, 128):
                rows = slice(p * HEAD_DIM + c, p * HEAD_DIM + c + 128)
                value = sum(ref[rows, :].astype(jnp.float32) * scale for ref, scale in zip(trio, scales))
                out_ref[tokens, RET_DIM + c : RET_DIM + c + 128] = jnp.transpose(
                    value * factor
                ).astype(jnp.bfloat16)


def finished(messages, gate, retained, pairs):
    tokens = retained.shape[0]
    return pl.pallas_call(
        functools.partial(final_kernel, pairs),
        out_shape=jax.ShapeDtypeStruct((tokens, RET_DIM + HEAD_DIM), jnp.bfloat16),
        in_specs=in_vmem(len(messages) + 2),
        out_specs=in_vmem(1)[0],
        compiler_params=limited(8),
        name="finish",
    )(*messages, gate, retained)


def body(
    tokens, ret_query, ret_key, ret_value, w_query, w_key, w_value, w_gate, store, passage_ids
):
    owners = lax.axis_size("st")
    chips = owners // 2
    far = chips // 2
    columns = lax.axis_size("tp")
    head = lax.axis_index("tp")
    mine = lax.axis_index("st")
    held = store.shape[0]
    half_tokens = tokens.shape[0] // 2
    pairs = half_tokens // PAIR

    def along(x, hops):
        return lax.ppermute(x, "st", [(i, (i + 2 * hops) % owners) for i in range(owners)])

    def across(x, hops):
        return lax.ppermute(x, "tp", [(i, (i + hops) % columns) for i in range(columns)])

    gate_weights = w_gate.T
    store_rows = store.reshape(-1, store.shape[2])
    partner = [(i, i ^ 1) for i in range(owners)]

    def extended(ids, reach):
        return jnp.concatenate([ids, along(ids, -reach)])

    first = tokens[:half_tokens]
    first_before, first_after = across(first, 1), across(first, -1)
    second = after(tokens, first)[half_tokens:]
    second_after = across(second, -1)
    ids = passage_ids.reshape(-1)
    ids = extended(ids, 1)
    key_own = jnp.dot(
        after(store_rows, second), w_key, preferred_element_type=jnp.float32
    ).astype(jnp.bfloat16)
    key_other = lax.ppermute(key_own, "st", partner)
    ids = extended(after(ids, key_own), 2)
    value_own = contracted(after(w_value, key_own), store_rows, (0, 1)).astype(jnp.bfloat16)
    value_other = lax.ppermute(value_own, "st", partner)
    first_before = after(first_before, value_own)
    first_opposite = across(first_before, 1)
    second_before = across(after(second, first_before), 1)
    ids = extended(after(ids, first_before), 4)
    second_opposite = across(second_after, -1)
    first_query, first_gate = project(
        head, [first, first_before, first_after, first_opposite], w_query, gate_weights
    )
    ids = extended(after(ids, first_query), 8)
    second_query, second_gate = project(
        head,
        [after(second, first_query), second_before, second_after, second_opposite],
        w_query,
        gate_weights,
    )
    queries = [first_query, second_query]
    gate = jnp.concatenate([first_gate, second_gate], 1)
    per_half = passage_ids.size // 2
    own_place = ids - mine * held
    other_place = ids - (mine ^ 1) * held
    table = jnp.where(
        (own_place >= 0) & (own_place < held),
        own_place,
        jnp.where((other_place >= 0) & (other_place < held), other_place + held, -1),
    )
    keys = jnp.concatenate([key_own, key_other], 0)
    values = jnp.concatenate([value_own, value_other], 1)

    def contribute(query, distance, half):
        offset = (distance % chips) * 2 * per_half + half * per_half
        return contribution(table, query, keys, values, offset, pairs)

    parts = [{0: contribute(queries[half], 0, half)} for half in range(2)]
    streams = [(half, way) for half in range(2) for way in (1, -1)]
    longest = {(0, 1): far, (0, -1): far - 1, (1, 1): far - 1, (1, -1): far}
    moving = {s: queries[s[0]] for s in streams}
    for hop in range(1, far + 1):
        for half, way in streams:
            if hop <= longest[half, way]:
                moving[half, way] = along(moving[half, way], way)
                distance = (-way * hop) % chips
                parts[half][distance] = contribute(moving[half, way], distance, half)

    back = {}
    for left in range(far, 0, -1):
        for half, way in streams:
            if left > longest[half, way]:
                continue
            own = parts[half][(way * left) % chips]
            if left == far - 3 and (half, way) == (0, 1):
                retained = retain(
                    retention_tables(head), after(ret_query, back[half, way]), ret_key, ret_value
                )
            back[half, way] = along(
                merged(back[half, way], own, pairs) if (half, way) in back else own, way
            )

    messages = []
    for half in range(2):
        messages += [back[half, 1], back[half, -1], parts[half][0]]
    return finished(messages, gate, retained, pairs)


def solution(mesh):
    placed = (
        P(("grp", "st"), "tp"),
        P(("grp", "st"), "tp"),
        P(("grp", "st"), "tp"),
        P(("grp", "st"), "tp"),
        P(None, "tp"),
        P(None, "tp"),
        P(None, "tp"),
        P(),
        P("st", None, None),
        P(("grp", "st"), None),
    )
    return jax.shard_map(
        body, mesh=mesh, in_specs=placed, out_specs=P(("grp", "st"), "tp"), check_vma=False
    )
```

```python
import functools

import jax
import jax.numpy as jnp
from jax import lax
from jax.experimental import pallas as pl
from jax.experimental.pallas import tpu as pltpu
from jax.sharding import PartitionSpec as P

RET_DIM = 256
HEAD_DIM = 512
BLOCK = 64
NPB = 4
SEQ_LEN = 256
PAIR = 2 * BLOCK
STATS = 16
LATER = 3
LOWEST = -(2.0**127)

ROTARY_BASE = 10000.0
NORM_EPS = 1e-05


MIB = 1024 * 1024


def limited(mib):
    return pltpu.CompilerParams(vmem_limit_bytes=mib * MIB)


def in_vmem(count):
    return [pl.BlockSpec(memory_space=pltpu.VMEM)] * count


def after(x, *others):
    return lax.optimization_barrier((x, *others))[0]


def contracted(left, right, dims):
    return lax.dot_general(left, right, ((dims[:1], dims[1:]), ((), ())), preferred_element_type=jnp.float32)


def retain_kernel(cos_ref, sin_ref, decay_ref, query_ref, key_ref, value_ref, out_ref):
    half = RET_DIM // 2
    cosines, sines = cos_ref[...], sin_ref[...]

    def rotated(ref):
        values = ref[...].astype(jnp.float32)
        leading, trailing = values[:, :half], values[:, half:]
        return jnp.concatenate(
            [leading * cosines - trailing * sines, leading * sines + trailing * cosines], axis=1
        )

    query = rotated(query_ref).astype(jnp.bfloat16)
    key = (rotated(key_ref) * RET_DIM ** (-0.5)).astype(jnp.bfloat16)
    weights = (contracted(query, key, (1, 1)) * decay_ref[...]).astype(jnp.bfloat16)
    output = jnp.dot(weights, value_ref[...], preferred_element_type=jnp.float32)
    centred = output - jnp.mean(output, -1, keepdims=True)
    out_ref[...] = (
        centred * lax.rsqrt(jnp.mean(centred * centred, -1, keepdims=True) + NORM_EPS)
    ).astype(jnp.bfloat16)


def retention_tables(head):
    places = jnp.arange(SEQ_LEN, dtype=jnp.int32)
    half = RET_DIM // 2
    inverse = ROTARY_BASE ** (-jnp.arange(half, dtype=jnp.float32) / half)
    angles = places.astype(jnp.float32)[:, None] * inverse
    log_gamma = jnp.log1p(-jnp.exp2(-5.0 - head.astype(jnp.float32)))
    offsets = (places[:, None] - places[None, :]).astype(jnp.float32)
    decay = jnp.where(offsets >= 0.0, jnp.exp(log_gamma * jnp.maximum(offsets, 0.0)), 0.0)
    return jnp.cos(angles), jnp.sin(angles), decay


def retain(tables, query_rows, key_rows, value_rows):
    rows = pl.BlockSpec((SEQ_LEN, RET_DIM), lambda i: (i, 0))
    half = pl.BlockSpec((SEQ_LEN, RET_DIM // 2), lambda i: (0, 0))
    return pl.pallas_call(
        retain_kernel,
        grid=(query_rows.shape[0] // SEQ_LEN,),
        out_shape=jax.ShapeDtypeStruct(query_rows.shape, jnp.bfloat16),
        in_specs=[half, half, pl.BlockSpec((SEQ_LEN, SEQ_LEN), lambda i: (0, 0)), rows, rows, rows],
        out_specs=rows,
        compiler_params=limited(8),
        cost_estimate=pl.CostEstimate(flops=4 * 10**9, transcendentals=0, bytes_accessed=10**6),
        name="retain",
    )(*tables, query_rows, key_rows, value_rows)


def project_kernel(aways, columns, last, head_ref, *refs):
    count = len(aways)
    piece_refs, weight_refs, gate_weight_ref = refs[:count], refs[count : 2 * count], refs[2 * count]
    total_ref, gates_ref = refs[-2:]
    features = piece_refs[0].shape[1]
    head = head_ref[0]
    total, gates = (refs[2 * count + 1][...], refs[2 * count + 2][...]) if last else (None, None)
    for piece_ref, weight_ref, away in zip(piece_refs, weight_refs, aways):
        at = pl.ds(pl.multiple_of(lax.rem(head + away, columns) * features, features), features)
        piece = piece_ref[...]
        part = jnp.dot(piece, weight_ref[...], preferred_element_type=jnp.float32)
        gate_part = contracted(gate_weight_ref[:, at], piece, (1, 1))
        total = part if total is None else total + part
        gates = gate_part if gates is None else gates + gate_part
    rows = total.shape[0]
    total_ref[:rows, :] = total.astype(total_ref.dtype)
    if total_ref.shape[0] > rows:
        total_ref[rows:, :] = refs[2 * count + 3][...]
    if last:
        which = lax.broadcasted_iota(jnp.int32, gates.shape, 0) == head
        gates = jax.nn.sigmoid(jnp.sum(jnp.where(which, gates, 0.0), 0, keepdims=True))
    gates_ref[...] = gates


def project(head, pieces, aways, weights, gate_weights, columns, so_far=(), tail=()):
    last = bool(so_far)
    rows, features = pieces[0].shape
    extra = tail[0].shape[0] if tail else 0
    width = weights.shape[1]

    def whole(x):
        return pl.BlockSpec(x.shape, lambda i, head_ref: (0, 0))

    def block(away):
        return pl.BlockSpec(
            (features, width), lambda i, head_ref: (lax.rem(head_ref[0] + away, columns), 0)
        )

    outs = (
        jax.ShapeDtypeStruct((rows + extra, width), jnp.bfloat16 if last else jnp.float32),
        jax.ShapeDtypeStruct((1 if last else columns, rows), jnp.float32),
    )
    return pl.pallas_call(
        functools.partial(project_kernel, aways, columns, last),
        out_shape=outs,
        grid_spec=pltpu.PrefetchScalarGridSpec(
            num_scalar_prefetch=1,
            grid=(1,),
            in_specs=[whole(x) for x in pieces]
            + [block(away) for away in aways]
            + [whole(x) for x in (gate_weights, *so_far, *tail)],
            out_specs=tuple(whole(x) for x in outs),
        ),
        compiler_params=limited(12),
        cost_estimate=pl.CostEstimate(flops=2 * 10**9, transcendentals=0, bytes_accessed=10**6),
        name="project",
    )(head.reshape(1), *pieces, *([weights] * len(pieces)), gate_weights, *so_far, *tail)


def split_three(row):
    high = row.astype(jnp.bfloat16).astype(jnp.float32)
    rest = row - high
    middle = rest.astype(jnp.bfloat16).astype(jnp.float32)
    return [high, middle, rest - middle]


def write_stats(out_ref, pairs, highest, totals):
    place = lax.broadcasted_iota(jnp.int32, (STATS, PAIR), 0)
    packed = jnp.zeros((STATS, PAIR), jnp.float32)
    row = 0
    for pair in range(pairs):
        for part in split_three(highest[pair]) + split_three(totals[pair]):
            packed = jnp.where(place == row, part, packed)
            row += 1
    out_ref[pairs * HEAD_DIM :, :] = packed.astype(jnp.bfloat16)


def read_stats(ref, pairs):
    packed = ref[pairs * HEAD_DIM :, :].astype(jnp.float32)
    rows = [packed[r : r + 1, :] for r in range(6 * pairs)]
    highest = [(rows[6 * p] + rows[6 * p + 1]) + rows[6 * p + 2] for p in range(pairs)]
    totals = [(rows[6 * p + 3] + rows[6 * p + 4]) + rows[6 * p + 5] for p in range(pairs)]
    return highest, totals


def contrib_kernel(starts, pairs, table_ref, key_ref, value_ref, *refs):
    count = len(starts)
    query_refs, out_refs, (high, tot) = refs[:count], refs[count : 2 * count], refs[2 * count :]
    lane_block = lax.broadcasted_iota(jnp.int32, (1, PAIR), 1) // BLOCK

    for start, query_ref, out_ref in zip(starts, query_refs, out_refs):
        high[...] = jnp.full_like(high, LOWEST)
        tot[...] = jnp.zeros_like(tot)

        def clear(i, carry, out_ref=out_ref):
            at = pl.ds(pl.multiple_of(i * 256, 256), 256)
            out_ref[at, :] = jnp.zeros((256, PAIR), jnp.bfloat16)
            return carry

        lax.fori_loop(0, pairs * HEAD_DIM // 256, clear, 0)

        def step(j, carry, start=start, query_ref=query_ref, out_ref=out_ref):
            passage = table_ref[start + j // NPB, j % NPB]

            @pl.when(passage >= 0)
            def _():
                pair = j // (2 * NPB)
                mine = lane_block == (j // NPB) % 2
                rows = pl.multiple_of(passage * 128, 128)
                scores = contracted(
                    key_ref[pl.ds(rows, 128), :],
                    query_ref[pl.ds(pl.multiple_of(pair * PAIR, PAIR), PAIR), :],
                    (1, 1),
                ) * HEAD_DIM ** (-0.5)
                top = jnp.max(scores, 0, keepdims=True)
                exponent = jnp.exp(scores - top)
                total = jnp.sum(exponent, 0, keepdims=True)
                weighted = jnp.dot(
                    value_ref[:, pl.ds(rows, 128)],
                    jnp.where(mine, exponent, 0.0).astype(jnp.bfloat16),
                    preferred_element_type=jnp.float32,
                )
                at = pl.ds(pl.multiple_of(pair * 8, 8), 1)
                old = high[at, :]
                new = jnp.where(mine, jnp.maximum(old, top), old)
                keep = jnp.exp(old - new)
                take = jnp.where(mine, jnp.exp(top - new), 0.0)
                where = pl.ds(pl.multiple_of(pair * HEAD_DIM, HEAD_DIM), HEAD_DIM)
                out_ref[where, :] = (
                    out_ref[where, :].astype(jnp.float32) * keep + weighted * take
                ).astype(jnp.bfloat16)
                high[at, :] = new
                tot[at, :] = tot[at, :] * keep + total * take

            return carry

        lax.fori_loop(0, 2 * pairs * NPB, step, 0)
        write_stats(
            out_ref,
            pairs,
            [high[8 * p : 8 * p + 1, :] for p in range(pairs)],
            [tot[8 * p : 8 * p + 1, :] for p in range(pairs)],
        )


def contributions(table, queries, keys, values, starts, pairs):
    out = jax.ShapeDtypeStruct((pairs * HEAD_DIM + STATS, PAIR), jnp.bfloat16)
    return pl.pallas_call(
        functools.partial(contrib_kernel, starts, pairs),
        out_shape=(out,) * len(queries),
        in_specs=[pl.BlockSpec(memory_space=pltpu.SMEM)] + in_vmem(2 + len(queries)),
        out_specs=tuple(in_vmem(len(queries))),
        scratch_shapes=[
            pltpu.VMEM((8 * pairs, PAIR), jnp.float32),
            pltpu.VMEM((8 * pairs, PAIR), jnp.float32),
        ],
        compiler_params=limited(8),
        cost_estimate=pl.CostEstimate(
            flops=4 * 10**9, transcendentals=10**5, bytes_accessed=10**6
        ),
        name="contributions",
    )(table, keys, values, *queries)


def merge_kernel(pairs, first_ref, second_ref, out_ref):
    high_a, tot_a = read_stats(first_ref, pairs)
    high_b, tot_b = read_stats(second_ref, pairs)
    highest, totals = [], []
    for p in range(pairs):
        top = jnp.maximum(high_a[p], high_b[p])
        scale_a, scale_b = jnp.exp(high_a[p] - top), jnp.exp(high_b[p] - top)

        def blend(i, carry, p=p, scale_a=scale_a, scale_b=scale_b):
            rows = pl.ds(pl.multiple_of(p * HEAD_DIM + i * 128, 128), 128)
            out_ref[rows, :] = (
                first_ref[rows, :].astype(jnp.float32) * scale_a
                + second_ref[rows, :].astype(jnp.float32) * scale_b
            ).astype(jnp.bfloat16)
            return carry

        lax.fori_loop(0, HEAD_DIM // 128, blend, 0)
        highest.append(top)
        totals.append(tot_a[p] * scale_a + tot_b[p] * scale_b)
    write_stats(out_ref, pairs, highest, totals)


def merged(first, second, pairs):
    return pl.pallas_call(
        functools.partial(merge_kernel, pairs),
        out_shape=jax.ShapeDtypeStruct(first.shape, first.dtype),
        in_specs=in_vmem(2),
        out_specs=in_vmem(1)[0],
        compiler_params=limited(2),
        cost_estimate=pl.CostEstimate(
            flops=10**9, transcendentals=10**4, bytes_accessed=10**6
        ),
        name="merge",
    )(first, second)


def final_kernel(pairs, *refs):
    message_refs, gate_ref, retained_ref, out_ref = refs[:-3], refs[-3], refs[-2], refs[-1]
    out_ref[:, :RET_DIM] = retained_ref[...]
    for half in range(len(message_refs) // 3):
        trio = message_refs[3 * half : 3 * half + 3]
        stats = [read_stats(ref, pairs) for ref in trio]
        for p in range(pairs):
            top = functools.reduce(jnp.maximum, [s[0][p] for s in stats])
            scales = [jnp.exp(s[0][p] - top) for s in stats]
            total = sum(s[1][p] * scale for s, scale in zip(stats, scales))
            tokens = slice((half * pairs + p) * PAIR, (half * pairs + p + 1) * PAIR)
            factor = gate_ref[:, tokens] / total
            for c in range(0, HEAD_DIM, 128):
                rows = slice(p * HEAD_DIM + c, p * HEAD_DIM + c + 128)
                value = sum(ref[rows, :].astype(jnp.float32) * scale for ref, scale in zip(trio, scales))
                out_ref[tokens, RET_DIM + c : RET_DIM + c + 128] = jnp.transpose(
                    value * factor
                ).astype(jnp.bfloat16)


def finished(messages, gate, retained, pairs):
    tokens = retained.shape[0]
    return pl.pallas_call(
        functools.partial(final_kernel, pairs),
        out_shape=jax.ShapeDtypeStruct((tokens, RET_DIM + HEAD_DIM), jnp.bfloat16),
        in_specs=in_vmem(len(messages) + 2),
        out_specs=in_vmem(1)[0],
        compiler_params=limited(8),
        name="finish",
    )(*messages, gate, retained)


def body(
    tokens, ret_query, ret_key, ret_value, w_query, w_key, w_value, w_gate, store, passage_ids
):
    owners = lax.axis_size("st")
    chips = owners // 2
    far = chips // 2
    columns = lax.axis_size("tp")
    head = lax.axis_index("tp")
    mine = lax.axis_index("st")
    held = store.shape[0]
    half_tokens = tokens.shape[0] // 2
    pairs = half_tokens // PAIR

    def along(x, hops):
        return lax.ppermute(x, "st", [(i, (i + 2 * hops) % owners) for i in range(owners)])

    def across(x, hops):
        return lax.ppermute(x, "tp", [(i, (i + hops) % columns) for i in range(columns)])

    gate_weights = w_gate.T
    store_rows = store.reshape(-1, store.shape[2])
    partner = [(i, i ^ 1) for i in range(owners)]

    blocks = passage_ids.shape[0]
    tail = jnp.pad(passage_ids.astype(jnp.bfloat16), ((0, 0), (0, HEAD_DIM - NPB)))

    def projected(pieces, opposite, started, tail=()):
        near = project(head, pieces, (0, columns - 1, 1), w_query, gate_weights, columns)
        return project(
            head,
            [after(opposite, started)],
            (columns // 2,),
            w_query,
            gate_weights,
            columns,
            near,
            tail,
        )

    def places(ids):
        own_place = ids - mine * held
        other_place = ids - (mine ^ 1) * held
        return jnp.where(
            (own_place >= 0) & (own_place < held),
            own_place,
            jnp.where((other_place >= 0) & (other_place < held), other_place + held, -1),
        )

    first = tokens[:half_tokens]
    first_before, first_after = across(first, 1), across(first, -1)
    second = after(tokens, first)[half_tokens:]
    second_after = across(second, -1)
    value_own = contracted(after(w_value, second), store_rows, (0, 1)).astype(jnp.bfloat16)
    value_other = lax.ppermute(value_own, "st", partner)
    first_before = after(first_before, value_own)
    first_opposite = across(first_before, 1)
    second_before = across(after(second, first_before), 1)
    second_opposite = across(second_after, -1)
    first_query, first_gate = projected(
        [first, after(first_before, second_after), first_after],
        first_opposite,
        second_after,
        (tail,),
    )
    key_own = jnp.dot(
        after(store_rows, first_query), w_key, preferred_element_type=jnp.float32
    ).astype(jnp.bfloat16)
    key_other = lax.ppermute(key_own, "st", partner)
    second_query, second_gate = projected(
        [after(second, key_own), second_before, second_after], second_opposite, second_before
    )
    queries = [first_query, second_query]
    gate = jnp.concatenate([first_gate, second_gate], 1)
    keys = jnp.concatenate([key_own, key_other], 0)
    values = jnp.concatenate([value_own, value_other], 1)

    def contribute(arrivals, table, moment=None):
        queries, starts = zip(*arrivals.values())
        if moment is not None:
            queries = (after(queries[0], moment), *queries[1:])
        outs = contributions(table, queries, keys, values, starts, pairs)
        return dict(zip(arrivals, outs))

    streams = [(half, way) for half in range(2) for way in (1, -1)]
    longest = {(0, 1): far, (0, -1): far - 1, (1, 1): far - 1, (1, -1): far}
    moving = {s: queries[s[0]] for s in streams}
    came, parts = {}, {}
    for hop in range(1, far + 1):
        for half, way in streams:
            if hop <= longest[half, way]:
                moving[half, way] = along(moving[half, way], way)
        ids = [
            moving[0, way][2 * pairs * BLOCK :, :NPB].astype(jnp.float32)
            for way in (1, -1)
            if hop <= longest[0, way]
        ]
        table = places(jnp.concatenate(ids, 0).astype(jnp.int32))
        arrivals = {
            (half, way): (
                moving[half, way],
                half * (blocks // 2) + (blocks * ((1 - way) // 2) if hop < far else 0),
            )
            for half, way in streams
            if hop <= longest[half, way]
        }
        came[hop] = (arrivals, table)
        if hop > LATER:
            parts[hop] = contribute(*came[hop])

    back = {}
    for left in range(far, 0, -1):
        if left not in parts:
            parts[left] = contribute(*came[left], back[0, 1, left + 2])
        for half, way in streams:
            if left > longest[half, way]:
                continue
            own = parts[left][half, way if left == far else -way]
            if left < longest[half, way]:
                own = merged(back[half, way, left + 1], own, pairs)
            back[half, way, left] = along(own, way)
            if left == far - 3 and (half, way) == (0, 1):
                retained = retain(
                    retention_tables(head), after(ret_query, back[half, way, left]), ret_key, ret_value
                )
    home = contribute(
        {half: (queries[half], half * (blocks // 2)) for half in range(2)},
        places(passage_ids),
        back[0, 1, 2],
    )

    messages = []
    for half in range(2):
        messages += [back[half, 1, 1], back[half, -1, 1], home[half]]
    return finished(messages, gate, retained, pairs)


def solution(mesh):
    placed = (
        P(("grp", "st"), "tp"),
        P(("grp", "st"), "tp"),
        P(("grp", "st"), "tp"),
        P(("grp", "st"), "tp"),
        P(None, "tp"),
        P(None, "tp"),
        P(None, "tp"),
        P(),
        P("st", None, None),
        P(("grp", "st"), None),
    )
    return jax.shard_map(
        body, mesh=mesh, in_specs=placed, out_specs=P(("grp", "st"), "tp"), check_vma=False
    )
```

```python
import functools

import jax
import jax.numpy as jnp
from jax import lax
from jax.experimental import pallas as pl
from jax.experimental.pallas import tpu as pltpu
from jax.sharding import PartitionSpec as P

RET_DIM = 256
HEAD_DIM = 512
BLOCK = 64
NPB = 4
SEQ_LEN = 256
PAIR = 2 * BLOCK
STATS = 16
LATER = 2
LOWEST = -(2.0**127)

ROTARY_BASE = 10000.0
NORM_EPS = 1e-05


MIB = 1024 * 1024


def limited(mib):
    return pltpu.CompilerParams(vmem_limit_bytes=mib * MIB)


def in_vmem(count):
    return [pl.BlockSpec(memory_space=pltpu.VMEM)] * count


def after(x, *others):
    return lax.optimization_barrier((x, *others))[0]


def contracted(left, right, dims):
    return lax.dot_general(left, right, ((dims[:1], dims[1:]), ((), ())), preferred_element_type=jnp.float32)


def retain_kernel(cos_ref, sin_ref, decay_ref, query_ref, key_ref, value_ref, out_ref):
    half = RET_DIM // 2
    cosines, sines = cos_ref[...], sin_ref[...]

    def rotated(ref):
        values = ref[...].astype(jnp.float32)
        leading, trailing = values[:, :half], values[:, half:]
        return jnp.concatenate(
            [leading * cosines - trailing * sines, leading * sines + trailing * cosines], axis=1
        )

    query = rotated(query_ref).astype(jnp.bfloat16)
    key = (rotated(key_ref) * RET_DIM ** (-0.5)).astype(jnp.bfloat16)
    weights = (contracted(query, key, (1, 1)) * decay_ref[...]).astype(jnp.bfloat16)
    output = jnp.dot(weights, value_ref[...], preferred_element_type=jnp.float32)
    centred = output - jnp.mean(output, -1, keepdims=True)
    out_ref[...] = (
        centred * lax.rsqrt(jnp.mean(centred * centred, -1, keepdims=True) + NORM_EPS)
    ).astype(jnp.bfloat16)


def retention_tables(head):
    places = jnp.arange(SEQ_LEN, dtype=jnp.int32)
    half = RET_DIM // 2
    inverse = ROTARY_BASE ** (-jnp.arange(half, dtype=jnp.float32) / half)
    angles = places.astype(jnp.float32)[:, None] * inverse
    log_gamma = jnp.log1p(-jnp.exp2(-5.0 - head.astype(jnp.float32)))
    offsets = (places[:, None] - places[None, :]).astype(jnp.float32)
    decay = jnp.where(offsets >= 0.0, jnp.exp(log_gamma * jnp.maximum(offsets, 0.0)), 0.0)
    return jnp.cos(angles), jnp.sin(angles), decay


def retain(tables, query_rows, key_rows, value_rows):
    rows = pl.BlockSpec((SEQ_LEN, RET_DIM), lambda i: (i, 0))
    half = pl.BlockSpec((SEQ_LEN, RET_DIM // 2), lambda i: (0, 0))
    return pl.pallas_call(
        retain_kernel,
        grid=(query_rows.shape[0] // SEQ_LEN,),
        out_shape=jax.ShapeDtypeStruct(query_rows.shape, jnp.bfloat16),
        in_specs=[half, half, pl.BlockSpec((SEQ_LEN, SEQ_LEN), lambda i: (0, 0)), rows, rows, rows],
        out_specs=rows,
        compiler_params=limited(8),
        cost_estimate=pl.CostEstimate(flops=4 * 10**9, transcendentals=0, bytes_accessed=10**6),
        name="retain",
    )(*tables, query_rows, key_rows, value_rows)


def project_kernel(aways, columns, last, head_ref, *refs):
    count = len(aways)
    piece_refs, weight_refs, gate_weight_ref = refs[:count], refs[count : 2 * count], refs[2 * count]
    total_ref, gates_ref = refs[-2:]
    features = piece_refs[0].shape[1]
    head = head_ref[0]
    total, gates = (refs[2 * count + 1][...], refs[2 * count + 2][...]) if last else (None, None)
    for piece_ref, weight_ref, away in zip(piece_refs, weight_refs, aways):
        at = pl.ds(pl.multiple_of(lax.rem(head + away, columns) * features, features), features)
        piece = piece_ref[...]
        part = jnp.dot(piece, weight_ref[...], preferred_element_type=jnp.float32)
        gate_part = contracted(gate_weight_ref[:, at], piece, (1, 1))
        total = part if total is None else total + part
        gates = gate_part if gates is None else gates + gate_part
    rows = total.shape[0]
    total_ref[:rows, :] = total.astype(total_ref.dtype)
    if total_ref.shape[0] > rows:
        total_ref[rows:, :] = refs[2 * count + 3][...]
    if last:
        which = lax.broadcasted_iota(jnp.int32, gates.shape, 0) == head
        gates = jax.nn.sigmoid(jnp.sum(jnp.where(which, gates, 0.0), 0, keepdims=True))
    gates_ref[...] = gates


def project(head, pieces, aways, weights, gate_weights, columns, so_far=(), tail=()):
    last = bool(so_far)
    rows, features = pieces[0].shape
    extra = tail[0].shape[0] if tail else 0
    width = weights.shape[1]

    def whole(x):
        return pl.BlockSpec(x.shape, lambda i, head_ref: (0, 0))

    def block(away):
        return pl.BlockSpec(
            (features, width), lambda i, head_ref: (lax.rem(head_ref[0] + away, columns), 0)
        )

    outs = (
        jax.ShapeDtypeStruct((rows + extra, width), jnp.bfloat16 if last else jnp.float32),
        jax.ShapeDtypeStruct((1 if last else columns, rows), jnp.float32),
    )
    return pl.pallas_call(
        functools.partial(project_kernel, aways, columns, last),
        out_shape=outs,
        grid_spec=pltpu.PrefetchScalarGridSpec(
            num_scalar_prefetch=1,
            grid=(1,),
            in_specs=[whole(x) for x in pieces]
            + [block(away) for away in aways]
            + [whole(x) for x in (gate_weights, *so_far, *tail)],
            out_specs=tuple(whole(x) for x in outs),
        ),
        compiler_params=limited(12),
        cost_estimate=pl.CostEstimate(flops=2 * 10**9, transcendentals=0, bytes_accessed=10**6),
        name="project",
    )(head.reshape(1), *pieces, *([weights] * len(pieces)), gate_weights, *so_far, *tail)


def table_kernel(held, first_row, where_ref, *refs):
    out_ref = refs[-1]
    own, other = where_ref[0] * held, where_ref[1] * held
    for k, ref in enumerate(refs[:-1]):
        ids = ref[first_row:, :128].astype(jnp.float32).astype(jnp.int32)[:, :NPB]
        own_place, other_place = ids - own, ids - other
        out_ref[k * ids.shape[0] : (k + 1) * ids.shape[0], :] = jnp.where(
            (own_place >= 0) & (own_place < held),
            own_place,
            jnp.where((other_place >= 0) & (other_place < held), other_place + held, -1),
        )


def tabulate(where, messages, held, first_row):
    blocks = messages[0].shape[0] - first_row
    return pl.pallas_call(
        functools.partial(table_kernel, held, first_row),
        out_shape=jax.ShapeDtypeStruct((len(messages) * blocks, NPB), jnp.int32),
        in_specs=[pl.BlockSpec(memory_space=pltpu.SMEM)] + in_vmem(len(messages)),
        out_specs=in_vmem(1)[0],
        compiler_params=limited(2),
        cost_estimate=pl.CostEstimate(flops=2 * 10**8, transcendentals=0, bytes_accessed=10**4),
        name="tabulate",
    )(where, *messages)


def split_three(row):
    high = row.astype(jnp.bfloat16).astype(jnp.float32)
    rest = row - high
    middle = rest.astype(jnp.bfloat16).astype(jnp.float32)
    return [high, middle, rest - middle]


def write_stats(out_ref, pairs, highest, totals):
    place = lax.broadcasted_iota(jnp.int32, (STATS, PAIR), 0)
    packed = jnp.zeros((STATS, PAIR), jnp.float32)
    row = 0
    for pair in range(pairs):
        for part in split_three(highest[pair]) + split_three(totals[pair]):
            packed = jnp.where(place == row, part, packed)
            row += 1
    out_ref[pairs * HEAD_DIM :, :] = packed.astype(jnp.bfloat16)


def read_stats(ref, pairs):
    packed = ref[pairs * HEAD_DIM :, :].astype(jnp.float32)
    rows = [packed[r : r + 1, :] for r in range(6 * pairs)]
    highest = [(rows[6 * p] + rows[6 * p + 1]) + rows[6 * p + 2] for p in range(pairs)]
    totals = [(rows[6 * p + 3] + rows[6 * p + 4]) + rows[6 * p + 5] for p in range(pairs)]
    return highest, totals


def contrib_kernel(starts, pairs, table_ref, key_ref, value_ref, *refs):
    count = len(starts)
    query_refs, out_refs, (high, tot) = refs[:count], refs[count : 2 * count], refs[2 * count :]
    lane_block = lax.broadcasted_iota(jnp.int32, (1, PAIR), 1) // BLOCK

    for start, query_ref, out_ref in zip(starts, query_refs, out_refs):
        high[...] = jnp.full_like(high, LOWEST)
        tot[...] = jnp.zeros_like(tot)

        def clear(i, carry, out_ref=out_ref):
            at = pl.ds(pl.multiple_of(i * 256, 256), 256)
            out_ref[at, :] = jnp.zeros((256, PAIR), jnp.bfloat16)
            return carry

        lax.fori_loop(0, pairs * HEAD_DIM // 256, clear, 0)

        def step(j, carry, start=start, query_ref=query_ref, out_ref=out_ref):
            passage = table_ref[start + j // NPB, j % NPB]

            @pl.when(passage >= 0)
            def _():
                pair = j // (2 * NPB)
                mine = lane_block == (j // NPB) % 2
                rows = pl.multiple_of(passage * 128, 128)
                scores = contracted(
                    key_ref[pl.ds(rows, 128), :],
                    query_ref[pl.ds(pl.multiple_of(pair * PAIR, PAIR), PAIR), :],
                    (1, 1),
                ) * HEAD_DIM ** (-0.5)
                top = jnp.max(scores, 0, keepdims=True)
                exponent = jnp.exp(scores - top)
                total = jnp.sum(exponent, 0, keepdims=True)
                weighted = jnp.dot(
                    value_ref[:, pl.ds(rows, 128)],
                    jnp.where(mine, exponent, 0.0).astype(jnp.bfloat16),
                    preferred_element_type=jnp.float32,
                )
                at = pl.ds(pl.multiple_of(pair * 8, 8), 1)
                old = high[at, :]
                new = jnp.where(mine, jnp.maximum(old, top), old)
                keep = jnp.exp(old - new)
                take = jnp.where(mine, jnp.exp(top - new), 0.0)
                where = pl.ds(pl.multiple_of(pair * HEAD_DIM, HEAD_DIM), HEAD_DIM)
                out_ref[where, :] = (
                    out_ref[where, :].astype(jnp.float32) * keep + weighted * take
                ).astype(jnp.bfloat16)
                high[at, :] = new
                tot[at, :] = tot[at, :] * keep + total * take

            return carry

        lax.fori_loop(0, 2 * pairs * NPB, step, 0)
        write_stats(
            out_ref,
            pairs,
            [high[8 * p : 8 * p + 1, :] for p in range(pairs)],
            [tot[8 * p : 8 * p + 1, :] for p in range(pairs)],
        )


def contributions(table, queries, keys, values, starts, pairs):
    out = jax.ShapeDtypeStruct((pairs * HEAD_DIM + STATS, PAIR), jnp.bfloat16)
    return pl.pallas_call(
        functools.partial(contrib_kernel, starts, pairs),
        out_shape=(out,) * len(queries),
        in_specs=[pl.BlockSpec(memory_space=pltpu.SMEM)] + in_vmem(2 + len(queries)),
        out_specs=tuple(in_vmem(len(queries))),
        scratch_shapes=[
            pltpu.VMEM((8 * pairs, PAIR), jnp.float32),
            pltpu.VMEM((8 * pairs, PAIR), jnp.float32),
        ],
        compiler_params=limited(8),
        cost_estimate=pl.CostEstimate(
            flops=4 * 10**9, transcendentals=10**5, bytes_accessed=10**6
        ),
        name="contributions",
    )(table, keys, values, *queries)


def merge_kernel(pairs, first_ref, second_ref, out_ref):
    high_a, tot_a = read_stats(first_ref, pairs)
    high_b, tot_b = read_stats(second_ref, pairs)
    highest, totals = [], []
    for p in range(pairs):
        top = jnp.maximum(high_a[p], high_b[p])
        scale_a, scale_b = jnp.exp(high_a[p] - top), jnp.exp(high_b[p] - top)

        def blend(i, carry, p=p, scale_a=scale_a, scale_b=scale_b):
            rows = pl.ds(pl.multiple_of(p * HEAD_DIM + i * 128, 128), 128)
            out_ref[rows, :] = (
                first_ref[rows, :].astype(jnp.float32) * scale_a
                + second_ref[rows, :].astype(jnp.float32) * scale_b
            ).astype(jnp.bfloat16)
            return carry

        lax.fori_loop(0, HEAD_DIM // 128, blend, 0)
        highest.append(top)
        totals.append(tot_a[p] * scale_a + tot_b[p] * scale_b)
    write_stats(out_ref, pairs, highest, totals)


def merged(first, second, pairs):
    return pl.pallas_call(
        functools.partial(merge_kernel, pairs),
        out_shape=jax.ShapeDtypeStruct(first.shape, first.dtype),
        in_specs=in_vmem(2),
        out_specs=in_vmem(1)[0],
        compiler_params=limited(2),
        cost_estimate=pl.CostEstimate(
            flops=10**9, transcendentals=10**4, bytes_accessed=10**6
        ),
        name="merge",
    )(first, second)


def final_kernel(pairs, *refs):
    message_refs, gate_ref, retained_ref, out_ref = refs[:-3], refs[-3], refs[-2], refs[-1]
    out_ref[:, :RET_DIM] = retained_ref[...]
    for half in range(len(message_refs) // 3):
        trio = message_refs[3 * half : 3 * half + 3]
        stats = [read_stats(ref, pairs) for ref in trio]
        for p in range(pairs):
            top = functools.reduce(jnp.maximum, [s[0][p] for s in stats])
            scales = [jnp.exp(s[0][p] - top) for s in stats]
            total = sum(s[1][p] * scale for s, scale in zip(stats, scales))
            tokens = slice((half * pairs + p) * PAIR, (half * pairs + p + 1) * PAIR)
            factor = gate_ref[:, tokens] / total
            for c in range(0, HEAD_DIM, 128):
                rows = slice(p * HEAD_DIM + c, p * HEAD_DIM + c + 128)
                value = sum(ref[rows, :].astype(jnp.float32) * scale for ref, scale in zip(trio, scales))
                out_ref[tokens, RET_DIM + c : RET_DIM + c + 128] = jnp.transpose(
                    value * factor
                ).astype(jnp.bfloat16)


def finished(messages, gate, retained, pairs):
    tokens = retained.shape[0]
    return pl.pallas_call(
        functools.partial(final_kernel, pairs),
        out_shape=jax.ShapeDtypeStruct((tokens, RET_DIM + HEAD_DIM), jnp.bfloat16),
        in_specs=in_vmem(len(messages) + 2),
        out_specs=in_vmem(1)[0],
        compiler_params=limited(8),
        name="finish",
    )(*messages, gate, retained)


def body(
    tokens, ret_query, ret_key, ret_value, w_query, w_key, w_value, w_gate, store, passage_ids
):
    owners = lax.axis_size("st")
    chips = owners // 2
    far = chips // 2
    columns = lax.axis_size("tp")
    head = lax.axis_index("tp")
    mine = lax.axis_index("st")
    held = store.shape[0]
    half_tokens = tokens.shape[0] // 2
    pairs = half_tokens // PAIR

    def along(x, hops):
        return lax.ppermute(x, "st", [(i, (i + 2 * hops) % owners) for i in range(owners)])

    def across(x, hops):
        return lax.ppermute(x, "tp", [(i, (i + hops) % columns) for i in range(columns)])

    gate_weights = w_gate.T
    store_rows = store.reshape(-1, store.shape[2])
    partner = [(i, i ^ 1) for i in range(owners)]

    blocks = passage_ids.shape[0]
    tail = jnp.pad(passage_ids.astype(jnp.bfloat16), ((0, 0), (0, HEAD_DIM - NPB)))

    def projected(pieces, opposite, started, tail=()):
        near = project(head, pieces, (0, columns - 1, 1), w_query, gate_weights, columns)
        return project(
            head,
            [after(opposite, started)],
            (columns // 2,),
            w_query,
            gate_weights,
            columns,
            near,
            tail,
        )

    def places(ids):
        own_place = ids - mine * held
        other_place = ids - (mine ^ 1) * held
        return jnp.where(
            (own_place >= 0) & (own_place < held),
            own_place,
            jnp.where((other_place >= 0) & (other_place < held), other_place + held, -1),
        )

    first = tokens[:half_tokens]
    first_before, first_after = across(first, 1), across(first, -1)
    second = after(tokens, first)[half_tokens:]
    second_after = across(second, -1)
    value_own = contracted(after(w_value, second), store_rows, (0, 1)).astype(jnp.bfloat16)
    value_other = lax.ppermute(value_own, "st", partner)
    first_before = after(first_before, value_own)
    first_opposite = across(first_before, 1)
    second_before = across(after(second, first_before), 1)
    second_opposite = across(second_after, -1)
    first_query, first_gate = projected(
        [first, first_before, first_after],
        first_opposite,
        second_after,
        (tail,),
    )
    key_own = jnp.dot(
        after(store_rows, first_query), w_key, preferred_element_type=jnp.float32
    ).astype(jnp.bfloat16)
    key_other = lax.ppermute(key_own, "st", partner)
    second_query, second_gate = projected(
        [after(second, key_own), second_before, second_after], second_opposite, second_before
    )
    queries = [first_query, second_query]
    gate = jnp.concatenate([first_gate, second_gate], 1)
    keys = jnp.concatenate([key_own, key_other], 0)
    values = jnp.concatenate([value_own, value_other], 1)

    def contribute(arrivals, table, moment=None):
        queries, starts = zip(*arrivals.values())
        if moment is not None:
            queries = (after(queries[0], moment), *queries[1:])
        outs = contributions(table, queries, keys, values, starts, pairs)
        return dict(zip(arrivals, outs))

    streams = [(half, way) for half in range(2) for way in (1, -1)]
    longest = {(0, 1): far, (0, -1): far - 1, (1, 1): far - 1, (1, -1): far}
    moving = {s: queries[s[0]] for s in streams}
    came, parts = {}, {}
    for hop in range(1, far + 1):
        for half, way in streams:
            if hop <= longest[half, way]:
                moving[half, way] = along(moving[half, way], way)
        table = tabulate(
            jnp.stack([mine, mine ^ 1]),
            [moving[0, way] for way in (1, -1) if hop <= longest[0, way]],
            held,
            2 * pairs * BLOCK,
        )
        arrivals = {
            (half, way): (
                moving[half, way],
                half * (blocks // 2) + (blocks * ((1 - way) // 2) if hop < far else 0),
            )
            for half, way in streams
            if hop <= longest[half, way]
        }
        came[hop] = (arrivals, table)
        if hop > LATER:
            parts[hop] = contribute(*came[hop])

    back = {}
    for left in range(far, 0, -1):
        if left not in parts:
            parts[left] = contribute(*came[left], back[0, 1, left + 2])
        for half, way in streams:
            if left > longest[half, way]:
                continue
            own = parts[left][half, way if left == far else -way]
            if left < longest[half, way]:
                own = merged(back[half, way, left + 1], own, pairs)
            back[half, way, left] = along(own, way)
            if left == far - 3 and (half, way) == (0, 1):
                retained = retain(
                    retention_tables(head), after(ret_query, back[half, way, left]), ret_key, ret_value
                )
    home = contribute(
        {half: (queries[half], half * (blocks // 2)) for half in range(2)},
        places(passage_ids),
        back[0, 1, 2],
    )

    messages = []
    for half in range(2):
        messages += [back[half, 1, 1], back[half, -1, 1], home[half]]
    return finished(messages, gate, retained, pairs)


def solution(mesh):
    placed = (
        P(("grp", "st"), "tp"),
        P(("grp", "st"), "tp"),
        P(("grp", "st"), "tp"),
        P(("grp", "st"), "tp"),
        P(None, "tp"),
        P(None, "tp"),
        P(None, "tp"),
        P(),
        P("st", None, None),
        P(("grp", "st"), None),
    )
    return jax.shard_map(
        body, mesh=mesh, in_specs=placed, out_specs=P(("grp", "st"), "tp"), check_vma=False
    )
```
